512 devices in a mesh: ep: 32 (over z, x), tp: 16 (over y, core).
Axes of the slice: x: 4, y: 8, z: 8, core: 2. Of those that a mesh axis runs over, the one named last changes fastest.
Arguments:
- queries: bfloat16 [196608, 1024], P(('ep', 'tp')), may hold values from -250 to 250
- keys_values: bfloat16 [2, 196608, 256], P(None, ('ep', 'tp')), may hold values from -8 to 8
- sink_logits: float32 [16], replicated, may hold values from 2 to 6
- moe_rows: bfloat16 [8192, 2048], P('ep'), may hold values from -600 to 600
- norm_gain: float32 [2048], replicated, may hold values from 0.1 to 1.9
- group_choice: int32 [8192], P('ep'), may hold values from 0 to 7, as said below
- member_choice: int32 [8192, 2], P('ep'), may hold values from 0 to 3, as said below
- route_weight: float32 [8192, 2], P('ep'), may hold values from 0.1 to 1
- w_gate: bfloat16 [32, 2048, 2048], P('ep', None, 'tp'), may hold values from -0.125 to 0.125
- w_up: bfloat16 [32, 2048, 2048], P('ep', None, 'tp'), may hold values from -0.125 to 0.125
- w_down: bfloat16 [32, 2048, 2048], P('ep', None, 'tp'), may hold values from -0.125 to 0.125
Outputs:
- attended: bfloat16 [196608, 1024], P(('ep', 'tp'))
- mixed: bfloat16 [8192, 2048], P('ep', 'tp')
The draws below stay inside these ranges and needn't reach their ends.
Inputs may be any that keep to these rules, and one draw needn't show every extreme that they name: With expert = group_choice * 4 + member_choice, within the 256 rows of one index of ep no expert is named by more than 32 rows, and some expert is named by exactly 32 rows. `member_choice`: the 2 entries of a row differ.
All inputs are finite; a program needn't handle non-finite values.
Results may differ from the reference program's by a relative error of at most 0.007.
Values may be sent and summed in bfloat16 or wider, within the bound.
A program may use at most 64 MiB of HBM per device.

```python
import math
import jax
import jax.numpy as jnp
from jax import lax

D = 2048
QH = 16
KVH = 4
HD = 64
WINDOW = 128
MOE_ROWS = 256
FF = 2048
EPG = 4
TOP = 2
EXPERTS = 32
ATOKENS = 196608
MOE_TOKENS = 8192
CAP = 32
N_EP = 32


def attention_pair(key):
    base_key = jax.random.fold_in(key, 101)
    seed_query, seed_keys, seed_value = jax.random.split(base_key, 3)
    queries = 1.5 * jax.random.normal(seed_query, (ATOKENS, QH * HD), jnp.float32)
    key_rows = jax.random.normal(seed_keys, (ATOKENS, KVH, HD), jnp.float32)
    values = 2.0 * jax.random.normal(seed_value, (ATOKENS, KVH * HD), jnp.float32)
    queries = jnp.clip(queries, -250.0, 250.0)
    stacked = jnp.clip(jnp.stack([key_rows.reshape(ATOKENS, KVH * HD), values]), -8.0, 8.0)
    return (queries.astype(jnp.bfloat16), stacked.astype(jnp.bfloat16))


def draw_queries(key, part):
    return attention_pair(key)[0]


def draw_keys_values(key, part):
    return attention_pair(key)[1]


def draw_moe_rows(key, part):
    base_key = jax.random.fold_in(key, 202)
    seed_rows, seed_columns, seed_noise = jax.random.split(base_key, 3)
    row_scale = jnp.exp(jax.random.uniform(seed_rows, (MOE_TOKENS, 1), jnp.float32, 0.0, math.log(10.0)))
    column_scale = jnp.exp(jax.random.uniform(seed_columns, (1, D), jnp.float32, 0.0, math.log(10.0)))
    values = row_scale * column_scale * jax.random.normal(seed_noise, (MOE_TOKENS, D), jnp.float32)
    return jnp.clip(values, -600.0, 600.0).astype(jnp.bfloat16)


def route_pair(key):
    base_key = jax.random.fold_in(key, 303)
    groups = EXPERTS // EPG
    seat_count = CAP * EPG // TOP
    star_rows = (CAP - 1) * EPG // TOP + 1
    others = MOE_ROWS - star_rows
    blocks = MOE_TOKENS // MOE_ROWS
    seed_star, seed_order, seed_blocks = jax.random.split(base_key, 3)
    star_group = jax.random.randint(seed_star, (), 0, groups)
    star_order = jax.random.permutation(seed_order, EPG)

    def one_block(block_key):
        seed_seat, seed_perm, seed_shuffle = jax.random.split(block_key, 3)
        seat_order = jax.random.permutation(seed_seat, (groups - 1) * seat_count)[:others]
        other_group = seat_order // seat_count
        other_group = other_group + (other_group >= star_group).astype(jnp.int32)
        group_all = jnp.concatenate([jnp.full((star_rows,), star_group, jnp.int32), other_group.astype(jnp.int32)])
        slot_all = jnp.concatenate([jnp.arange(star_rows, dtype=jnp.int32), (seat_order % seat_count).astype(jnp.int32)])
        orders = jax.vmap(lambda seed_one: jax.random.permutation(seed_one, EPG))(jax.random.split(seed_perm, groups))
        orders = jnp.where((jnp.arange(groups) == star_group)[:, None], star_order[None, :], orders)
        columns = (TOP * slot_all[:, None] + jnp.arange(TOP, dtype=jnp.int32)[None, :]) % EPG
        members = orders[group_all[:, None], columns]
        shuffle = jax.random.permutation(seed_shuffle, MOE_ROWS)
        return (group_all[shuffle], members[shuffle])
    group_out, member_out = jax.vmap(one_block)(jax.random.split(seed_blocks, blocks))
    return (group_out.reshape(MOE_TOKENS).astype(jnp.int32), member_out.reshape(MOE_TOKENS, TOP).astype(jnp.int32))


def draw_group_choice(key, part):
    return route_pair(key)[0]


def draw_member_choice(key, part):
    return route_pair(key)[1]


def level_of(key, extent, pieces, least, high):
    loudness = 1.0
    for dim, shards_of in pieces:
        steps = jax.random.uniform(jax.random.fold_in(jax.random.fold_in(key, 6), dim), (shards_of,), jnp.float32, least / len(pieces), high / len(pieces))
        loudness = loudness * jnp.repeat(jnp.exp(steps), extent[dim] // shards_of).reshape((-1,) + (1,) * (len(extent) - 1 - dim))
    return loudness


def bell_draw(key, dims, scale, limit, cuts=(), kind=jnp.bfloat16):
    values = jax.random.normal(key, dims, jnp.float32) * scale
    if len(cuts) > 0:
        values = level_of(key, dims, cuts, -0.22, 0.18) * values
    return jnp.clip(values, min=-limit, max=limit).astype(kind)


def setup_inputs(seed: int = 0) -> dict:
    keys = jax.random.split(jax.random.key(seed), 12)
    queries = draw_queries(jax.random.fold_in(keys[11], 71), 0)
    keys_values = draw_keys_values(jax.random.fold_in(keys[11], 71), 0)
    sink_logits = jnp.clip(jax.random.uniform(keys[2], (QH,), jnp.float32, 2.0, 6.0), 2.0, 6.0)
    moe_rows = draw_moe_rows(jax.random.fold_in(keys[11], 71), 0)
    norm_gain = jnp.clip(1.0 + 0.18 * jax.random.normal(keys[4], (D,), jnp.float32), 0.1, 1.9)
    group_choice = draw_group_choice(jax.random.fold_in(keys[11], 71), 0)
    member_choice = draw_member_choice(jax.random.fold_in(keys[11], 71), 0)
    route_weight = jnp.clip(0.1 + 0.9 * jax.random.uniform(keys[7], (MOE_TOKENS, TOP), jnp.float32) ** level_of(keys[7], (MOE_TOKENS, TOP), ((0, 32),), -0.2, 0.2), 0.1, 1.0)
    w_gate = bell_draw(keys[8], (EXPERTS, D, FF), D ** -0.5, 0.125, ((0, 32), (2, 16)))
    w_up = bell_draw(keys[9], (EXPERTS, D, FF), D ** -0.5, 0.125, ((0, 32), (2, 16)))
    w_down = bell_draw(keys[10], (EXPERTS, FF, D), FF ** -0.5, 0.125, ((0, 32), (2, 16)))
    return {"queries": queries, "keys_values": keys_values, "sink_logits": sink_logits, "moe_rows": moe_rows, "norm_gain": norm_gain, "group_choice": group_choice, "member_choice": member_choice, "route_weight": route_weight, "w_gate": w_gate, "w_up": w_up, "w_down": w_down}


def attend_all(queries, keys_values, sink_logits):
    sharing = QH // KVH
    blocks = ATOKENS // WINDOW
    padded = jnp.pad(keys_values, ((0, 0), (WINDOW, 0), (0, 0)))
    first_half = padded[:, :ATOKENS].reshape(2, blocks, WINDOW, KVH, HD)
    second_half = padded[:, WINDOW:].reshape(2, blocks, WINDOW, KVH, HD)
    banded = jnp.concatenate([first_half, second_half], axis=2)
    query_blocks = queries.reshape(blocks, WINDOW, KVH, sharing, HD)
    key_column = jnp.arange(2 * WINDOW, dtype=jnp.int32)
    distance = jnp.arange(WINDOW, dtype=jnp.int32)[:, None] + WINDOW - key_column[None, :]
    inside = (distance >= 0) & (distance < WINDOW)
    sink_column = sink_logits.reshape(KVH, sharing)[:, :, None]

    def one_block(operands):
        query_block, key_block, value_block, number = operands
        scores = jnp.einsum('qhgd,khd->hgqk', query_block.astype(jnp.float32), key_block.astype(jnp.float32)) * HD ** (-0.5)
        visible = inside & (number * WINDOW + key_column[None, :] - WINDOW >= 0)
        scores = jnp.where(visible[None, None], scores, -1e+30)
        highest = jnp.maximum(lax.optimization_barrier(jnp.max(scores, axis=-1)), sink_column)
        weights = jnp.exp(scores - highest[..., None])
        totals = lax.optimization_barrier(jnp.sum(weights, axis=-1)) + jnp.exp(sink_column - highest)
        rounded = lax.optimization_barrier(weights.astype(jnp.bfloat16)).astype(jnp.float32)
        summed = jnp.einsum('hgqk,khd->qhgd', rounded, value_block.astype(jnp.float32))
        return (summed / jnp.transpose(totals, (2, 0, 1))[..., None]).astype(jnp.bfloat16)
    result = lax.map(one_block, (query_blocks, banded[0], banded[1], jnp.arange(blocks, dtype=jnp.int32)))
    return result.reshape(ATOKENS, QH * HD)

def experts_all(moe_rows, norm_gain, group_choice, member_choice, route_weight, w_gate, w_up, w_down):
    values = moe_rows.astype(jnp.float32)
    normed = (values * lax.rsqrt(lax.optimization_barrier(jnp.mean(values * values, axis=1, keepdims=True)) + 1e-06) * norm_gain).astype(jnp.bfloat16)
    chosen = (group_choice[:, None] * EPG + member_choice).astype(jnp.int32).reshape(N_EP, MOE_ROWS * TOP)
    onehot = (chosen[:, :, None] == jnp.arange(EXPERTS, dtype=jnp.int32)[None, None, :]).astype(jnp.int32)
    earlier = (jnp.cumsum(onehot, axis=1) - onehot).astype(jnp.int32)
    position = lax.optimization_barrier(jnp.sum(earlier * onehot, axis=2)).astype(jnp.int32)
    source = jnp.arange(N_EP, dtype=jnp.int32)[:, None]
    placed = (chosen * (N_EP * CAP) + source * CAP + position).astype(jnp.int32).reshape(MOE_TOKENS, TOP)
    source_row = jnp.arange(MOE_TOKENS * TOP, dtype=jnp.int32) // TOP
    lookup = jnp.full((EXPERTS * N_EP * CAP,), MOE_TOKENS, jnp.int32).at[placed.reshape(-1)].set(source_row)
    padded = jnp.concatenate([normed, jnp.zeros((1, D), jnp.bfloat16)], axis=0)

    def one_expert(operands):
        row_index, gate_weight, up_weight, down_weight = operands
        inputs = padded[row_index]
        gate_part = jnp.dot(inputs, gate_weight, preferred_element_type=jnp.float32)
        up_part = jnp.dot(inputs, up_weight, preferred_element_type=jnp.float32)
        hidden = (jax.nn.silu(gate_part) * up_part).astype(jnp.bfloat16)
        return jnp.dot(hidden, down_weight, preferred_element_type=jnp.float32).astype(jnp.bfloat16)
    produced = lax.map(one_expert, (lookup.reshape(EXPERTS, N_EP * CAP), w_gate, w_up, w_down))
    picked = produced.reshape(EXPERTS * N_EP * CAP, D)[placed].astype(jnp.float32)
    return lax.optimization_barrier(jnp.sum(route_weight[:, :, None] * picked, axis=1)).astype(jnp.bfloat16)

def reference(queries, keys_values, sink_logits, moe_rows, norm_gain, group_choice, member_choice, route_weight, w_gate, w_up, w_down):
    attended = attend_all(queries, keys_values, sink_logits)
    mixed = experts_all(moe_rows, norm_gain, group_choice, member_choice, route_weight, w_gate, w_up, w_down)
    return (attended, mixed)
```

```python
import functools

import jax
import jax.numpy as jnp
from jax import lax
from jax.experimental import pallas as pl
from jax.experimental.pallas import tpu as pltpu
from jax.sharding import PartitionSpec as P

QH = 16
KVH = 4
HD = 64
WINDOW = 128
EPG = 4
CAP = 32
HALF = CAP // 2
CW = 256
NSUB = 4

F32 = jnp.float32
BF16 = jnp.bfloat16


def iota(shape, dim):
    return lax.broadcasted_iota(jnp.int32, shape, dim)


def dot(a, b):
    return jnp.dot(a, b, preferred_element_type=F32)


def dot_t(a, b):
    return lax.dot_general(a, b, (((1,), (1,)), ((), ())), preferred_element_type=F32)


def kernel(
    n_ep,
    n_tp,
    q_hbm,
    kv_hbm,
    sink_ref,
    rows_hbm,
    gain_ref,
    chosen_ref,
    weight_ref,
    wg_hbm,
    wu_hbm,
    wd_hbm,
    att_hbm,
    mix_ref,
    rows_v,
    q_v,
    kv_v,
    wgu,
    wd,
    outb,
    xbuf,
    hbuf,
    acc,
    acc2,
    obuf,
    rbuf,
    att_v,
    pick,
    maskb,
    loc_sem,
    w_send,
    w_recv,
    edge_sem,
    d_send,
    d_recv,
    ring_send,
    ring_recv,
    r_send,
    r_recv,
):
    ep = lax.axis_index("ep")
    tp = lax.axis_index("tp")
    c = lax.rem(tp, 2)
    y = lax.div(tp, 2)
    ny = n_tp // 2
    steps = ny // 2
    slots = n_ep * HALF
    sr = slots // NSUB
    per_sub = n_ep // NSUB
    length = q_v.shape[0]
    blocks = length // WINDOW
    tokens = rows_v.shape[0]
    width = rows_v.shape[1]
    right = lax.rem(y + 1, ny)
    left = lax.rem(y + ny - 1, ny)

    def device(e, t):
        return {"ep": e, "tp": t}

    load_rows = pltpu.make_async_copy(rows_hbm, rows_v, loc_sem.at[0])
    load_q = pltpu.make_async_copy(q_hbm, q_v, loc_sem.at[1])
    load_kv = pltpu.make_async_copy(kv_hbm, kv_v.at[:, pl.ds(WINDOW, length), :], loc_sem.at[2])
    load_rows.start()
    load_q.start()
    load_kv.start()
    mine = pl.ds(pl.multiple_of(c * 128, 128), 128)
    mine_up = pl.ds(pl.multiple_of(c * 128 + CW, 128), 128)
    weight_ends = (
        (wg_hbm.at[0], wgu.at[:, mine]),
        (wu_hbm.at[0], wgu.at[:, mine_up]),
        (wd_hbm.at[0], wd.at[:, mine]),
    )
    load_w = [
        pltpu.make_async_copy(src, dst, loc_sem.at[3 + i]) for i, (src, dst) in enumerate(weight_ends)
    ]
    for copy in load_w:
        copy.start()

    barrier = pltpu.get_barrier_semaphore()
    plane = 2 * n_ep
    here = ep * 2 + c

    def greet(r, carry):
        other = lax.rem(here + r, plane)
        pl.semaphore_signal(
            barrier, inc=1, device_id=device(lax.div(other, 2), 2 * y + lax.rem(other, 2))
        )
        return carry

    lax.fori_loop(1, plane, greet, 0)
    pl.semaphore_signal(barrier, inc=1, device_id=device(ep, 2 * right + c))
    pl.semaphore_signal(barrier, inc=1, device_id=device(ep, 2 * left + c))
    flat = ep * n_tp + tp
    total = n_ep * n_tp
    after = lax.rem(flat + 1, total)
    before = lax.rem(flat + total - 1, total)
    after_dev = device(lax.div(after, n_tp), lax.rem(after, n_tp))
    pl.semaphore_signal(barrier, inc=1, device_id=after_dev)
    pl.semaphore_signal(
        barrier, inc=1, device_id=device(lax.div(before, n_tp), lax.rem(before, n_tp))
    )

    chosen = chosen_ref[...]
    lanes = iota((tokens, 128), 1)
    named = [chosen[:, k : k + 1] == lanes for k in range(2)]
    either = jnp.where(named[0] | named[1], 1.0, 0.0)
    lower = jnp.where(iota((tokens, tokens), 1) < iota((tokens, tokens), 0), 1.0, 0.0).astype(BF16)
    position = dot(lower, either.astype(BF16))
    spread = jnp.where(either > 0.5, position, -1.0).astype(BF16)
    repeat = jnp.where(
        lax.div(iota((slots, 128), 0), HALF) == iota((slots, 128), 1), 1.0, 0.0
    ).astype(BF16)
    wanted = (lax.rem(iota((slots, tokens), 0), HALF) + c * HALF).astype(F32)
    seats = jnp.where(dot_t(repeat, spread) == wanted, 1.0, 0.0).astype(BF16)

    load_rows.wait()
    square = jnp.zeros((tokens, 128), F32)
    for i in range(width // 128):
        part = rows_v[:, i * 128 : (i + 1) * 128].astype(F32)
        square = square + part * part
    mean = jnp.sum(square, axis=1, keepdims=True) * (1.0 / width)
    columns = pl.ds(pl.multiple_of(y * CW, CW), CW)
    normed = (
        rows_v[:, columns].astype(F32) * lax.rsqrt(mean + 1e-06) * gain_ref[:, columns]
    ).astype(BF16)
    outb[...] = dot(seats, normed).astype(BF16)

    pl.semaphore_wait(barrier, plane - 1 + 4)

    my_rows = pl.ds(pl.multiple_of(ep * HALF, HALF), HALF)
    my_sub = lax.div(ep, per_sub)

    def dispatch(r, carry):
        e = lax.rem(ep + r, n_ep)
        pltpu.make_async_remote_copy(
            src_ref=outb.at[pl.ds(pl.multiple_of(e * HALF, HALF), HALF)],
            dst_ref=xbuf.at[y, my_rows],
            send_sem=d_send.at[0],
            recv_sem=d_recv.at[my_sub],
            device_id=device(e, tp),
        ).start()
        return carry

    lax.fori_loop(1, n_ep, dispatch, 0)
    pltpu.make_async_copy(outb.at[my_rows], xbuf.at[y, my_rows], d_recv.at[my_sub]).start()

    edge = pltpu.make_async_remote_copy(
        src_ref=kv_hbm.at[:, pl.ds(length - WINDOW, WINDOW), :],
        dst_ref=kv_v.at[:, pl.ds(0, WINDOW), :],
        send_sem=edge_sem.at[0],
        recv_sem=edge_sem.at[1],
        device_id=after_dev,
    )
    edge.start()
    partner = device(ep, 2 * y + 1 - c)
    share_w = [
        pltpu.make_async_remote_copy(
            src_ref=src,
            dst_ref=dst,
            send_sem=w_send.at[i],
            recv_sem=w_recv.at[i],
            device_id=partner,
        )
        for i, (src, dst) in enumerate(weight_ends)
    ]
    for copy in share_w:
        copy.start()

    for k in range(2):
        seat = jnp.sum(jnp.where(named[k], position, 0.0), axis=1, keepdims=True)
        place = chosen[:, k : k + 1] * CAP + seat.astype(jnp.int32)
        pick[k] = jnp.where(place == iota((tokens, n_ep * CAP), 1), 1.0, 0.0).astype(BF16)

    gap = lax.rem(iota((2 * WINDOW, 2 * WINDOW), 0), WINDOW) + WINDOW - iota((2 * WINDOW, 2 * WINDOW), 1)
    maskb[...] = jnp.where((gap >= 0) & (gap < WINDOW), 0.0, -1e30)
    load_q.wait()
    load_kv.wait()

    def attend(b, p):
        rows = pl.ds(pl.multiple_of(b * WINDOW, WINDOW), WINDOW)
        key_rows = pl.ds(pl.multiple_of(b * WINDOW, WINDOW), 2 * WINDOW)
        pair = pl.ds(pl.multiple_of(p * 128, 128), 128)
        keys = kv_v[0, key_rows, pair]
        vals = kv_v[1, key_rows, pair]
        low_lane = iota((2 * WINDOW, 128), 1) < HD
        swap = jnp.where(
            lax.rem(iota((128, 128), 0) + HD, 128) == iota((128, 128), 1), 1.0, 0.0
        ).astype(BF16)
        zero = jnp.zeros((2 * WINDOW, 128), BF16)
        keys_sw = dot(keys, swap).astype(BF16)
        vals_sw = dot(vals, swap).astype(BF16)
        start = jnp.where((b == 0) & (flat == 0), -1e30, 0.0)
        visible = maskb[...] + jnp.where(iota((1, 2 * WINDOW), 1) < WINDOW, start, 0.0)
        for h in range(2):
            k_low, k_high = (keys, keys_sw) if h == 0 else (keys_sw, keys)
            v_low, v_high = (vals, vals_sw) if h == 0 else (vals_sw, vals)
            k_half = (jnp.where(low_lane, k_low, zero), jnp.where(low_lane, zero, k_high))
            v_half = (jnp.where(low_lane, v_low, zero), jnp.where(low_lane, zero, v_high))
            at = p * (8 * HD) + h * (4 * HD)
            tiles = [pl.ds(pl.multiple_of(at + i * 128, 128), 128) for i in range(2)]
            query = jnp.concatenate([q_v[rows, t] for t in tiles], axis=0)
            summed = None
            totals = []
            for i in range(2):
                scores = dot_t(query, k_half[i]) * (HD**-0.5) + visible
                head = p * 8 + h * 4 + i
                sink = jnp.where(
                    iota((2 * WINDOW, 1), 0) < WINDOW, sink_ref[head], sink_ref[head + 2]
                )
                highest = jnp.maximum(jnp.max(scores, axis=1, keepdims=True), sink)
                weights = jnp.exp(scores - highest)
                totals.append(jnp.sum(weights, axis=1, keepdims=True) + jnp.exp(sink - highest))
                part = dot(weights.astype(BF16), v_half[i])
                summed = part if summed is None else summed + part
            out = (summed / jnp.where(low_lane, totals[0], totals[1])).astype(BF16)
            for i in range(2):
                att_v[rows, tiles[i]] = out[i * WINDOW : (i + 1) * WINDOW]

    def attend_block(b):
        def body(p, carry):
            attend(b, p)
            return carry

        lax.fori_loop(0, 2, body, 0)

    def attend_tail(b, carry):
        attend_block(b)
        return carry

    lax.fori_loop(1, blocks, attend_tail, 0)

    def piece(buf, phase, way, t, sub, incoming):
        hop = t + 1 if incoming else t
        chunk = lax.rem(y + (ny - hop if way == 0 else hop), ny)
        part = buf.at[chunk, pl.ds(sub * sr, sr)]
        target = right if way == 0 else left
        return pltpu.make_async_remote_copy(
            src_ref=part,
            dst_ref=part,
            send_sem=ring_send.at[phase, way, t, sub],
            recv_sem=ring_recv.at[phase, way, t, sub],
            device_id=device(ep, 2 * target + c),
        )

    def travels(way, t, sub):
        return t < steps - 1 or (sub < NSUB // 2) == (way == 0)

    def add_chunk(buf, weights, total_ref, chunk, first):
        depth = weights[pl.ds(pl.multiple_of(chunk * CW, CW), CW), :]
        big = slots // 2

        def body(i, carry):
            rows = pl.ds(pl.multiple_of(i * big, big), big)
            value = dot(buf[chunk, rows], depth)
            if first:
                total_ref[rows, :] = value
            else:
                total_ref[rows, :] += value
            return carry

        lax.fori_loop(0, 2, body, 0)

    def ring(buf, weights, total_ref, phase, between):
        add_chunk(buf, weights, total_ref, y, True)
        for t in range(steps - 1):
            between(t)
            for sub in range(NSUB):
                for way in range(2):
                    piece(buf, phase, way, t, sub, True).wait_recv()
                    if travels(way, t + 1, sub):
                        piece(buf, phase, way, t + 1, sub, False).start()
            add_chunk(buf, weights, total_ref, lax.rem(y + ny - t - 1, ny), False)
            add_chunk(buf, weights, total_ref, lax.rem(y + t + 1, ny), False)

    def last_pieces(buf, phase, sub):
        way = 0 if sub < NSUB // 2 else 1
        piece(buf, phase, way, steps - 1, sub, True).wait_recv()

    far = lax.rem(y + steps, ny)
    far_rows = pl.ds(pl.multiple_of(far * CW, CW), CW)
    order = [sub for pair in zip(range(NSUB // 2), range(NSUB // 2, NSUB)) for sub in pair]

    for sub in range(NSUB):
        held = xbuf.at[y, pl.ds(sub * sr, sr)]
        pltpu.make_async_copy(held, held, d_recv.at[sub]).wait()
        for way in range(2):
            if travels(way, 0, sub):
                piece(xbuf, 0, way, 0, sub, False).start()
    for i in range(2):
        load_w[i].wait()
        share_w[i].wait_recv()

    def spare(t):
        if t == 0:
            edge.wait_recv()
            attend_block(0)
            pltpu.make_async_copy(att_v, att_hbm, loc_sem.at[6]).start()

    ring(xbuf, wgu, acc, 0, spare)
    for sub in order:
        rows = pl.ds(sub * sr, sr)
        last_pieces(xbuf, 0, sub)
        both = acc[rows, :] + dot(xbuf[far, rows], wgu[far_rows, :])
        gate = both[:, :CW]
        hbuf[y, rows] = (gate / (1.0 + jnp.exp(-gate)) * both[:, CW:]).astype(BF16)
        for way in range(2):
            if travels(way, 0, sub):
                piece(hbuf, 1, way, 0, sub, False).start()
    load_w[2].wait()
    share_w[2].wait_recv()
    ring(hbuf, wd, acc2, 1, lambda t: None)

    back_rows = pl.ds(pl.multiple_of(ep * CAP + c * HALF, HALF), HALF)
    for sub in order:
        rows = pl.ds(sub * sr, sr)
        last_pieces(hbuf, 1, sub)
        obuf[rows, :] = (acc2[rows, :] + dot(hbuf[far, rows], wd[far_rows, :])).astype(BF16)

        def give_back(i, carry):
            s = sub * per_sub + i
            from_rows = pl.ds(pl.multiple_of(s * HALF, HALF), HALF)
            theirs = pl.ds(pl.multiple_of((1 - c) * 128, 128), 128)
            pltpu.make_async_remote_copy(
                src_ref=obuf.at[from_rows, theirs],
                dst_ref=rbuf.at[back_rows],
                send_sem=r_send.at[0],
                recv_sem=r_recv.at[0],
                device_id=device(s, 2 * y + 1 - c),
            ).start()

            @pl.when(s != ep)
            def _():
                pltpu.make_async_remote_copy(
                    src_ref=obuf.at[from_rows, mine],
                    dst_ref=rbuf.at[back_rows],
                    send_sem=r_send.at[1],
                    recv_sem=r_recv.at[0],
                    device_id=device(s, tp),
                ).start()

            @pl.when(s == ep)
            def _():
                pltpu.make_async_copy(
                    obuf.at[from_rows, mine], rbuf.at[back_rows], r_recv.at[0]
                ).start()

            return carry

        lax.fori_loop(0, per_sub, give_back, 0)

    for phase, buf in ((0, xbuf), (1, hbuf)):
        for way in range(2):
            for t in range(steps):
                for sub in range(NSUB):
                    if travels(way, t, sub):
                        piece(buf, phase, way, t, sub, False).wait_send()
    sent = outb.at[pl.ds(0, slots - HALF)]
    pltpu.make_async_copy(sent, sent, d_send.at[0]).wait()
    edge.wait_send()
    for copy in share_w:
        copy.wait_send()
    pltpu.make_async_copy(att_v, att_hbm, loc_sem.at[6]).wait()

    pltpu.make_async_copy(rbuf, rbuf, r_recv.at[0]).wait()
    mixed = weight_ref[:, 0:1] * dot(pick[0], rbuf[...])
    mixed = mixed + weight_ref[:, 1:2] * dot(pick[1], rbuf[...])
    mix_ref[...] = mixed.astype(BF16)

    back = obuf.at[:, pl.ds(0, 128)]
    pltpu.make_async_copy(back, back, r_send.at[0]).wait()
    back_less = obuf.at[pl.ds(0, slots - HALF), pl.ds(0, 128)]
    pltpu.make_async_copy(back_less, back_less, r_send.at[1]).wait()


def shards(
    n_ep,
    n_tp,
    queries,
    keys_values,
    sink_logits,
    moe_rows,
    norm_gain,
    group_choice,
    member_choice,
    route_weight,
    w_gate,
    w_up,
    w_down,
):
    tokens, width = moe_rows.shape
    length = queries.shape[0]
    slots = n_ep * HALF
    ny = n_tp // 2
    steps = ny // 2
    chosen = group_choice[:, None] * EPG + member_choice
    hbm = pl.BlockSpec(memory_space=pl.ANY)
    vmem = pl.BlockSpec(memory_space=pltpu.VMEM)
    smem = pl.BlockSpec(memory_space=pltpu.SMEM)
    dma = pltpu.SemaphoreType.DMA
    return pl.pallas_call(
        functools.partial(kernel, n_ep, n_tp),
        out_shape=(
            jax.ShapeDtypeStruct(queries.shape, BF16),
            jax.ShapeDtypeStruct((tokens, 128), BF16),
        ),
        in_specs=[hbm, hbm, smem, hbm, vmem, vmem, vmem, hbm, hbm, hbm],
        out_specs=(hbm, vmem),
        scratch_shapes=[
            pltpu.VMEM((tokens, width), BF16),
            pltpu.VMEM((length, QH * HD), BF16),
            pltpu.VMEM((2, length + WINDOW, KVH * HD), BF16),
            pltpu.VMEM((width, 2 * CW), BF16),
            pltpu.VMEM((width, CW), BF16),
            pltpu.VMEM((slots, CW), BF16),
            pltpu.VMEM((ny, slots, CW), BF16),
            pltpu.VMEM((ny, slots, CW), BF16),
            pltpu.VMEM((slots, 2 * CW), F32),
            pltpu.VMEM((slots, CW), F32),
            pltpu.VMEM((slots, CW), BF16),
            pltpu.VMEM((n_ep * CAP, 128), BF16),
            pltpu.VMEM((length, QH * HD), BF16),
            pltpu.VMEM((2, tokens, n_ep * CAP), BF16),
            pltpu.VMEM((2 * WINDOW, 2 * WINDOW), F32),
            dma((7,)),
            dma((3,)),
            dma((3,)),
            dma((2,)),
            dma((1,)),
            dma((NSUB,)),
            dma((2, 2, steps, NSUB)),
            dma((2, 2, steps, NSUB)),
            dma((2,)),
            dma((1,)),
        ],
        compiler_params=pltpu.CompilerParams(
            collective_id=0, has_side_effects=True, vmem_limit_bytes=50 * 2**20
        ),
        name="step",
    )(
        queries,
        keys_values,
        sink_logits,
        moe_rows,
        norm_gain.reshape(1, width),
        chosen,
        route_weight,
        w_gate,
        w_up,
        w_down,
    )


def solution(mesh):
    in_specs = (
        P(("ep", "tp"), None),
        P(None, ("ep", "tp"), None),
        P(),
        P("ep", None),
        P(),
        P("ep"),
        P("ep", None),
        P("ep", None),
        P("ep", None, "tp"),
        P("ep", None, "tp"),
        P("ep", None, "tp"),
    )
    out_specs = (P(("ep", "tp"), None), P("ep", "tp"))
    body = functools.partial(shards, mesh.shape["ep"], mesh.shape["tp"])
    return jax.shard_map(body, mesh=mesh, in_specs=in_specs, out_specs=out_specs, check_vma=False)
```

```python
import functools

import jax
import jax.numpy as jnp
from jax import lax
from jax.experimental import pallas as pl
from jax.experimental.pallas import tpu as pltpu
from jax.sharding import PartitionSpec as P

QH = 16
KVH = 4
HD = 64
WINDOW = 128
EPG = 4
CAP = 32
HALF = CAP // 2
CW = 256
NSUB = 4

F32 = jnp.float32
BF16 = jnp.bfloat16


def iota(shape, dim):
    return lax.broadcasted_iota(jnp.int32, shape, dim)


def dot(a, b):
    return jnp.dot(a, b, preferred_element_type=F32)


def dot_t(a, b):
    return lax.dot_general(a, b, (((1,), (1,)), ((), ())), preferred_element_type=F32)


def kernel(
    n_ep,
    n_tp,
    q_hbm,
    kv_hbm,
    sink_hbm,
    rows_hbm,
    gain_hbm,
    group_hbm,
    member_hbm,
    weight_hbm,
    wg_hbm,
    wu_hbm,
    wd_hbm,
    att_out,
    mix_ref,
    sink_ref,
    gain_ref,
    group_ref,
    member_ref,
    weight_ref,
    rows_v,
    q_v,
    kv_v,
    wgu,
    wd,
    outb,
    xbuf,
    hbuf,
    acc,
    acc2,
    obuf,
    rbuf,
    att_v,
    pick,
    maskb,
    share,
    loc_sem,
    w_send,
    w_recv,
    edge_sem,
    d_send,
    d_recv,
    ring_send,
    ring_recv,
    r_send,
    r_recv,
):
    ep = lax.axis_index("ep")
    tp = lax.axis_index("tp")
    c = lax.rem(tp, 2)
    y = lax.div(tp, 2)
    ny = n_tp // 2
    steps = ny // 2
    slots = n_ep * HALF
    sr = slots // NSUB
    per_sub = n_ep // NSUB
    length = q_v.shape[0]
    blocks = length // WINDOW
    tokens = rows_v.shape[0]
    width = rows_v.shape[1]
    right = lax.rem(y + 1, ny)
    left = lax.rem(y + ny - 1, ny)

    def device(e, t):
        return {"ep": e, "tp": t}

    load_rows = pltpu.make_async_copy(rows_hbm, rows_v, loc_sem.at[0])
    load_q = pltpu.make_async_copy(q_hbm, q_v, loc_sem.at[1])
    load_kv = pltpu.make_async_copy(kv_hbm, kv_v.at[:, pl.ds(WINDOW, length), :], loc_sem.at[2])
    small = [
        pltpu.make_async_copy(src, dst, loc_sem.at[7 + i])
        for i, (src, dst) in enumerate(
            (
                (group_hbm, group_ref),
                (member_hbm, member_ref),
                (gain_hbm, gain_ref),
                (weight_hbm, weight_ref),
                (sink_hbm, sink_ref),
            )
        )
    ]
    for copy in small:
        copy.start()
    load_rows.start()
    load_q.start()
    load_kv.start()
    mine = pl.ds(pl.multiple_of(c * 128, 128), 128)
    mine_up = pl.ds(pl.multiple_of(c * 128 + CW, 128), 128)
    weight_ends = (
        (wg_hbm.at[0], wgu.at[:, mine]),
        (wu_hbm.at[0], wgu.at[:, mine_up]),
        (wd_hbm.at[0], wd.at[:, mine]),
    )
    load_w = [
        pltpu.make_async_copy(src, dst, loc_sem.at[3 + i]) for i, (src, dst) in enumerate(weight_ends)
    ]
    for copy in load_w:
        copy.start()

    barrier = pltpu.get_barrier_semaphore()
    plane = 2 * n_ep
    here = ep * 2 + c

    def greet(r, carry):
        other = lax.rem(here + r, plane)
        pl.semaphore_signal(
            barrier, inc=1, device_id=device(lax.div(other, 2), 2 * y + lax.rem(other, 2))
        )
        return carry

    with jax.named_scope("greet"):
        lax.fori_loop(1, plane, greet, 0)
    pl.semaphore_signal(barrier, inc=1, device_id=device(ep, 2 * right + c))
    pl.semaphore_signal(barrier, inc=1, device_id=device(ep, 2 * left + c))
    flat = ep * n_tp + tp
    total = n_ep * n_tp
    after = lax.rem(flat + 1, total)
    before = lax.rem(flat + total - 1, total)
    after_dev = device(lax.div(after, n_tp), lax.rem(after, n_tp))
    pl.semaphore_signal(barrier, inc=1, device_id=after_dev)
    pl.semaphore_signal(
        barrier, inc=1, device_id=device(lax.div(before, n_tp), lax.rem(before, n_tp))
    )

    with jax.named_scope("routing"):
        small[0].wait()
        small[1].wait()
        chosen = group_ref[...] * EPG + member_ref[...]
        experts = iota((128, tokens), 0)
        named = [chosen[k : k + 1, :] == experts for k in range(2)]
        either = named[0] | named[1]
        upper = jnp.where(
            iota((tokens, tokens), 0) < iota((tokens, tokens), 1), 1.0, 0.0
        ).astype(BF16)
        position = dot(jnp.where(either, 1.0, 0.0).astype(BF16), upper)
        spread = jnp.where(either, position, -1.0).astype(BF16)
        repeat = jnp.where(
            lax.div(iota((slots, 128), 0), HALF) == iota((slots, 128), 1), 1.0, 0.0
        ).astype(BF16)
        wanted = (lax.rem(iota((slots, tokens), 0), HALF) + c * HALF).astype(F32)
        seats = jnp.where(dot(repeat, spread) == wanted, 1.0, 0.0).astype(BF16)

    with jax.named_scope("norm"):
        load_rows.wait()
        small[2].wait()
        square = jnp.zeros((tokens, 128), F32)
        for i in range(width // 128):
            part = rows_v[:, i * 128 : (i + 1) * 128].astype(F32)
            square = square + part * part
        mean = jnp.sum(square, axis=1, keepdims=True) * (1.0 / width)
        columns = pl.ds(pl.multiple_of(y * CW, CW), CW)
        normed = (
            rows_v[:, columns].astype(F32) * lax.rsqrt(mean + 1e-06) * gain_ref[:, columns]
        ).astype(BF16)
        outb[...] = dot(seats, normed).astype(BF16)

    with jax.named_scope("barrier"):
        pl.semaphore_wait(barrier, plane - 1 + 4)

    def offset(j):
        return jnp.where(lax.rem(j, 2) == 1, lax.div(j + 1, 2), lax.rem(n_ep - lax.div(j, 2), n_ep))

    def block(j):
        return pl.ds(pl.multiple_of(j * HALF, HALF), HALF)

    def dispatch(j, carry):
        e = lax.rem(ep + offset(j), n_ep)
        pltpu.make_async_remote_copy(
            src_ref=outb.at[block(e)],
            dst_ref=xbuf.at[y, block(j)],
            send_sem=d_send.at[0],
            recv_sem=d_recv.at[lax.div(j, per_sub)],
            device_id=device(e, tp),
        ).start()
        return carry

    with jax.named_scope("dispatch"):
        lax.fori_loop(1, n_ep, dispatch, 0)
        pltpu.make_async_copy(outb.at[block(ep)], xbuf.at[y, block(0)], d_recv.at[0]).start()

    edge = pltpu.make_async_remote_copy(
        src_ref=kv_hbm.at[:, pl.ds(length - WINDOW, WINDOW), :],
        dst_ref=kv_v.at[:, pl.ds(0, WINDOW), :],
        send_sem=edge_sem.at[0],
        recv_sem=edge_sem.at[1],
        device_id=after_dev,
    )
    edge.start()
    partner = device(ep, 2 * y + 1 - c)
    share_w = [
        pltpu.make_async_remote_copy(
            src_ref=src,
            dst_ref=dst,
            send_sem=w_send.at[i],
            recv_sem=w_recv.at[i],
            device_id=partner,
        )
        for i, (src, dst) in enumerate(weight_ends)
    ]
    with jax.named_scope("shares"):
        for copy in share_w:
            copy.start()

    with jax.named_scope("pick"):
        small[3].wait()
        sheet = [weight_ref[...]]
        for k in range(2):
            seat = jnp.sum(jnp.where(named[k], position, 0.0), axis=0, keepdims=True)
            sheet.append(chosen[k : k + 1, :].astype(F32) * CAP + seat)
        sheet.append(jnp.zeros((4, tokens), F32))
        upright = jnp.concatenate(sheet, axis=0).T
        share[...] = upright
        for k in range(2):
            place = upright[:, 2 + k : 3 + k].astype(jnp.int32)
            pick[k] = jnp.where(place == iota((tokens, n_ep * CAP), 1), 1.0, 0.0).astype(BF16)

    gap = lax.rem(iota((2 * WINDOW, 2 * WINDOW), 0), WINDOW) + WINDOW - iota((2 * WINDOW, 2 * WINDOW), 1)
    maskb[...] = jnp.where((gap >= 0) & (gap < WINDOW), 0.0, -1e30)
    with jax.named_scope("loads"):
        load_q.wait()
        load_kv.wait()
        small[4].wait()

    def attend(b, p):
        rows = pl.ds(pl.multiple_of(b * WINDOW, WINDOW), WINDOW)
        key_rows = pl.ds(pl.multiple_of(b * WINDOW, WINDOW), 2 * WINDOW)
        pair = pl.ds(pl.multiple_of(p * 128, 128), 128)
        keys = kv_v[0, key_rows, pair]
        vals = kv_v[1, key_rows, pair]
        low_lane = iota((2 * WINDOW, 128), 1) < HD
        swap = jnp.where(
            lax.rem(iota((128, 128), 0) + HD, 128) == iota((128, 128), 1), 1.0, 0.0
        ).astype(BF16)
        zero = jnp.zeros((2 * WINDOW, 128), BF16)
        keys_sw = dot(keys, swap).astype(BF16)
        vals_sw = dot(vals, swap).astype(BF16)
        start = jnp.where((b == 0) & (flat == 0), -1e30, 0.0)
        visible = maskb[...] + jnp.where(iota((1, 2 * WINDOW), 1) < WINDOW, start, 0.0)
        for h in range(2):
            k_low, k_high = (keys, keys_sw) if h == 0 else (keys_sw, keys)
            v_low, v_high = (vals, vals_sw) if h == 0 else (vals_sw, vals)
            k_half = (jnp.where(low_lane, k_low, zero), jnp.where(low_lane, zero, k_high))
            v_half = (jnp.where(low_lane, v_low, zero), jnp.where(low_lane, zero, v_high))
            at = p * (8 * HD) + h * (4 * HD)
            tiles = [pl.ds(pl.multiple_of(at + i * 128, 128), 128) for i in range(2)]
            query = jnp.concatenate([q_v[rows, t] for t in tiles], axis=0)
            summed = None
            totals = []
            for i in range(2):
                scores = dot_t(query, k_half[i]) * (HD**-0.5) + visible
                head = p * 8 + h * 4 + i
                sink = jnp.where(
                    iota((2 * WINDOW, 1), 0) < WINDOW, sink_ref[head], sink_ref[head + 2]
                )
                highest = jnp.maximum(jnp.max(scores, axis=1, keepdims=True), sink)
                weights = jnp.exp(scores - highest)
                totals.append(jnp.sum(weights, axis=1, keepdims=True) + jnp.exp(sink - highest))
                part = dot(weights.astype(BF16), v_half[i])
                summed = part if summed is None else summed + part
            out = (summed / jnp.where(low_lane, totals[0], totals[1])).astype(BF16)
            for i in range(2):
                att_v[rows, tiles[i]] = out[i * WINDOW : (i + 1) * WINDOW]

    def attend_tail(i, carry):
        attend(1 + lax.div(i, 2), lax.rem(i, 2))
        return carry

    with jax.named_scope("attend"):
        lax.fori_loop(0, 2 * (blocks - 1), attend_tail, 0)

    def piece(buf, phase, way, t, sub, incoming):
        hop = t + 1 if incoming else t
        chunk = lax.rem(y + (ny - hop if way == 0 else hop), ny)
        part = buf.at[chunk, pl.ds(sub * sr, sr)]
        target = right if way == 0 else left
        return pltpu.make_async_remote_copy(
            src_ref=part,
            dst_ref=part,
            send_sem=ring_send.at[phase, way, t, sub],
            recv_sem=ring_recv.at[phase, way, t, sub],
            device_id=device(ep, 2 * target + c),
        )

    def travels(way, t, sub):
        return t < steps - 1 or (sub % 2 == 0) == (way == 0)

    def send(buf, phase, t, sub):
        for way in range(2):
            if travels(way, t, sub):
                piece(buf, phase, way, t, sub, False).start()

    def add_chunk(buf, weights, total_ref, chunk, first=False):
        value = dot(buf[chunk], weights[pl.ds(pl.multiple_of(chunk * CW, CW), CW), :])
        if first:
            total_ref[...] = value
        else:
            total_ref[...] += value

    def ring(buf, weights, total_ref, phase, between):
        add_chunk(buf, weights, total_ref, y, True)
        for t in range(steps - 1):
            for sub in range(NSUB):
                for way in range(2):
                    piece(buf, phase, way, t, sub, True).wait_recv()
                    if travels(way, t + 1, sub):
                        piece(buf, phase, way, t + 1, sub, False).start()
            between(t)
            add_chunk(buf, weights, total_ref, lax.rem(y + ny - t - 1, ny))
            add_chunk(buf, weights, total_ref, lax.rem(y + t + 1, ny))

    def last_piece(buf, phase, sub):
        way = 0 if travels(0, steps - 1, sub) else 1
        piece(buf, phase, way, steps - 1, sub, True).wait_recv()

    far = lax.rem(y + steps, ny)
    far_rows = pl.ds(pl.multiple_of(far * CW, CW), CW)

    def hide(sub):
        last_piece(xbuf, 0, sub)
        rows = pl.ds(sub * sr, sr)
        both = acc[rows, :] + dot(xbuf[far, rows], wgu[far_rows, :])
        gate = both[:, :CW]
        hbuf[y, rows] = (gate / (1.0 + jnp.exp(-gate)) * both[:, CW:]).astype(BF16)
        send(hbuf, 1, 0, sub)

    def give_back(j, carry):
        s = lax.rem(ep + n_ep - offset(j), n_ep)
        theirs = pl.ds(pl.multiple_of((1 - c) * 128, 128), 128)
        pltpu.make_async_remote_copy(
            src_ref=obuf.at[block(j), theirs],
            dst_ref=rbuf.at[back_rows],
            send_sem=r_send.at[0],
            recv_sem=r_recv.at[0],
            device_id=device(s, 2 * y + 1 - c),
        ).start()

        @pl.when(s != ep)
        def _():
            pltpu.make_async_remote_copy(
                src_ref=obuf.at[block(j), mine],
                dst_ref=rbuf.at[back_rows],
                send_sem=r_send.at[1],
                recv_sem=r_recv.at[0],
                device_id=device(s, tp),
            ).start()

        @pl.when(s == ep)
        def _():
            pltpu.make_async_copy(
                obuf.at[block(j), mine], rbuf.at[back_rows], r_recv.at[0]
            ).start()

        return carry

    back_rows = pl.ds(pl.multiple_of(ep * CAP + c * HALF, HALF), HALF)

    def finish(sub):
        last_piece(hbuf, 1, sub)
        rows = pl.ds(sub * sr, sr)
        obuf[rows, :] = (acc2[rows, :] + dot(hbuf[far, rows], wd[far_rows, :])).astype(BF16)
        lax.fori_loop(sub * per_sub, (sub + 1) * per_sub, give_back, 0)

    def arrive(sub):
        held = xbuf.at[y, pl.ds(sub * sr, sr)]
        pltpu.make_async_copy(held, held, d_recv.at[sub]).wait()
        send(xbuf, 0, 0, sub)

    def early(t):
        if t == 0:
            edge.wait_recv()
        for p in range(2):
            if t == min(p, steps - 2):
                attend(0, p)
        if t == steps - 2:
            pltpu.make_async_copy(att_v, att_out, loc_sem.at[6]).start()

    with jax.named_scope("arrive"):
        for sub in range(NSUB):
            arrive(sub)
    with jax.named_scope("weights"):
        for i in range(2):
            load_w[i].wait()
            share_w[i].wait_recv()
    with jax.named_scope("ringx"):
        ring(xbuf, wgu, acc, 0, early)
    with jax.named_scope("middle"):
        for sub in range(NSUB):
            hide(sub)
    load_w[2].wait()
    share_w[2].wait_recv()
    with jax.named_scope("ringh"):
        ring(hbuf, wd, acc2, 1, lambda t: None)
    with jax.named_scope("down"):
        for sub in range(NSUB):
            finish(sub)

    with jax.named_scope("close"):
        for phase, buf in ((0, xbuf), (1, hbuf)):
            for way in range(2):
                for t in range(steps):
                    for sub in range(NSUB):
                        if travels(way, t, sub):
                            piece(buf, phase, way, t, sub, False).wait_send()
        sent = outb.at[pl.ds(0, slots - HALF)]
        pltpu.make_async_copy(sent, sent, d_send.at[0]).wait()
        edge.wait_send()
        for copy in share_w:
            copy.wait_send()
        pltpu.make_async_copy(att_v, att_out, loc_sem.at[6]).wait()

    with jax.named_scope("home"):
        pltpu.make_async_copy(rbuf, rbuf, r_recv.at[0]).wait()
    with jax.named_scope("mix"):
        mixed = share[:, 0:1] * dot(pick[0], rbuf[...])
        mixed = mixed + share[:, 1:2] * dot(pick[1], rbuf[...])
        mix_ref[...] = mixed.astype(BF16)

    back = obuf.at[:, pl.ds(0, 128)]
    pltpu.make_async_copy(back, back, r_send.at[0]).wait()
    back_less = obuf.at[pl.ds(0, slots - HALF), pl.ds(0, 128)]
    pltpu.make_async_copy(back_less, back_less, r_send.at[1]).wait()


def hand_on(att_in, mix_in, att_out, mix_out, att_v, mix_v, sem):
    pieces = 4
    size = att_v.shape[0] // pieces
    ways = [(mix_in, mix_v, mix_out)]
    for i in range(pieces):
        part = pl.ds(i * size, size)
        ways.append((att_in.at[part], att_v.at[part], att_out.at[part]))
    loads = [pltpu.make_async_copy(a, b, sem.at[0, i]) for i, (a, b, _) in enumerate(ways)]
    stores = [pltpu.make_async_copy(b, c, sem.at[1, i]) for i, (_, b, c) in enumerate(ways)]
    for load in loads:
        load.start()
    for load, store in zip(loads, stores):
        load.wait()
        store.start()
    for store in stores:
        store.wait()


def shards(
    n_ep,
    n_tp,
    queries,
    keys_values,
    sink_logits,
    moe_rows,
    norm_gain,
    group_choice,
    member_choice,
    route_weight,
    w_gate,
    w_up,
    w_down,
):
    tokens, width = moe_rows.shape
    length = queries.shape[0]
    slots = n_ep * HALF
    ny = n_tp // 2
    steps = ny // 2
    hbm = pl.BlockSpec(memory_space=pl.ANY)
    vmem = pl.BlockSpec(memory_space=pltpu.VMEM)
    dma = pltpu.SemaphoreType.DMA
    attended, mixed = pl.pallas_call(
        functools.partial(kernel, n_ep, n_tp),
        out_shape=(
            jax.ShapeDtypeStruct(queries.shape, BF16),
            jax.ShapeDtypeStruct((tokens, 128), BF16),
        ),
        in_specs=[hbm] * 11,
        out_specs=(hbm, vmem),
        scratch_shapes=[
            pltpu.SMEM((QH,), F32),
            pltpu.VMEM((1, width), F32),
            pltpu.VMEM((1, tokens), jnp.int32),
            pltpu.VMEM((2, tokens), jnp.int32),
            pltpu.VMEM((2, tokens), F32),
            pltpu.VMEM((tokens, width), BF16),
            pltpu.VMEM((length, QH * HD), BF16),
            pltpu.VMEM((2, length + WINDOW, KVH * HD), BF16),
            pltpu.VMEM((width, 2 * CW), BF16),
            pltpu.VMEM((width, CW), BF16),
            pltpu.VMEM((slots, CW), BF16),
            pltpu.VMEM((ny, slots, CW), BF16),
            pltpu.VMEM((ny, slots, CW), BF16),
            pltpu.VMEM((slots, 2 * CW), F32),
            pltpu.VMEM((slots, CW), F32),
            pltpu.VMEM((slots, CW), BF16),
            pltpu.VMEM((n_ep * CAP, 128), BF16),
            pltpu.VMEM((length, QH * HD), BF16),
            pltpu.VMEM((2, tokens, n_ep * CAP), BF16),
            pltpu.VMEM((2 * WINDOW, 2 * WINDOW), F32),
            pltpu.VMEM((tokens, 8), F32),
            dma((12,)),
            dma((3,)),
            dma((3,)),
            dma((2,)),
            dma((1,)),
            dma((NSUB,)),
            dma((2, 2, steps, NSUB)),
            dma((2, 2, steps, NSUB)),
            dma((2,)),
            dma((1,)),
        ],
        compiler_params=pltpu.CompilerParams(
            collective_id=0, has_side_effects=True, vmem_limit_bytes=66900000
        ),
        name="step",
    )(
        queries,
        keys_values,
        sink_logits,
        moe_rows,
        norm_gain.reshape(1, width),
        group_choice.reshape(1, tokens),
        member_choice.T,
        route_weight.T,
        w_gate,
        w_up,
        w_down,
    )
    return pl.pallas_call(
        hand_on,
        out_shape=(
            jax.ShapeDtypeStruct(attended.shape, BF16),
            jax.ShapeDtypeStruct(mixed.shape, BF16),
        ),
        in_specs=[hbm, hbm],
        out_specs=(hbm, hbm),
        scratch_shapes=[
            pltpu.VMEM(attended.shape, BF16),
            pltpu.VMEM(mixed.shape, BF16),
            dma((2, 5)),
        ],
        compiler_params=pltpu.CompilerParams(vmem_limit_bytes=66900000),
        name="hand_on",
    )(attended, mixed)


def solution(mesh):
    in_specs = (
        P(("ep", "tp"), None),
        P(None, ("ep", "tp"), None),
        P(),
        P("ep", None),
        P(),
        P("ep"),
        P("ep", None),
        P("ep", None),
        P("ep", None, "tp"),
        P("ep", None, "tp"),
        P("ep", None, "tp"),
    )
    out_specs = (P(("ep", "tp"), None), P("ep", "tp"))
    body = functools.partial(shards, mesh.shape["ep"], mesh.shape["tp"])
    return jax.shard_map(body, mesh=mesh, in_specs=in_specs, out_specs=out_specs, check_vma=False)
```

```python
import functools

import jax
import jax.numpy as jnp
from jax import lax
from jax.experimental import pallas as pl
from jax.experimental.pallas import tpu as pltpu
from jax.sharding import PartitionSpec as P

QH = 16
KVH = 4
HD = 64
WINDOW = 128
EPG = 4
CAP = 32
HALF = CAP // 2
CW = 256
NSUB = 4

F32 = jnp.float32
BF16 = jnp.bfloat16


def iota(shape, dim):
    return lax.broadcasted_iota(jnp.int32, shape, dim)


def dot(a, b):
    return jnp.dot(a, b, preferred_element_type=F32)


def dot_t(a, b):
    return lax.dot_general(a, b, (((1,), (1,)), ((), ())), preferred_element_type=F32)


def kernel(
    n_ep,
    n_tp,
    q_hbm,
    kv_hbm,
    sink_hbm,
    rows_hbm,
    gain_hbm,
    group_hbm,
    member_hbm,
    weight_hbm,
    wg_hbm,
    wu_hbm,
    wd_hbm,
    att_out,
    rbuf,
    sheet_out,
    sink_ref,
    gain_ref,
    group_ref,
    member_ref,
    weight_ref,
    rows_v,
    q_v,
    kv_v,
    wgu,
    wd,
    outb,
    xbuf,
    hbuf,
    acc,
    acc2,
    obuf,
    att_v,
    maskb,
    sheet_v,
    loc_sem,
    w_send,
    w_recv,
    edge_sem,
    d_send,
    d_recv,
    ring_send,
    ring_recv,
    r_send,
    r_recv,
):
    ep = lax.axis_index("ep")
    tp = lax.axis_index("tp")
    c = lax.rem(tp, 2)
    y = lax.div(tp, 2)
    ny = n_tp // 2
    steps = ny // 2
    slots = n_ep * HALF
    sr = slots // NSUB
    per_sub = n_ep // NSUB
    length = q_v.shape[0]
    blocks = length // WINDOW
    tokens = rows_v.shape[0]
    width = rows_v.shape[1]
    right = lax.rem(y + 1, ny)
    left = lax.rem(y + ny - 1, ny)

    def device(e, t):
        return {"ep": e, "tp": t}

    load_rows = pltpu.make_async_copy(rows_hbm, rows_v, loc_sem.at[0])
    load_q = pltpu.make_async_copy(q_hbm, q_v, loc_sem.at[1])
    load_kv = pltpu.make_async_copy(kv_hbm, kv_v.at[:, pl.ds(WINDOW, length), :], loc_sem.at[2])
    small = [
        pltpu.make_async_copy(src, dst, loc_sem.at[7 + i])
        for i, (src, dst) in enumerate(
            (
                (group_hbm, group_ref),
                (member_hbm, member_ref),
                (gain_hbm, gain_ref),
                (weight_hbm, weight_ref),
                (sink_hbm, sink_ref),
            )
        )
    ]
    for copy in small:
        copy.start()
    load_rows.start()
    load_q.start()
    load_kv.start()
    mine = pl.ds(pl.multiple_of(c * 128, 128), 128)
    mine_up = pl.ds(pl.multiple_of(c * 128 + CW, 128), 128)
    weight_ends = (
        (wg_hbm.at[0], wgu.at[:, mine]),
        (wu_hbm.at[0], wgu.at[:, mine_up]),
        (wd_hbm.at[0], wd.at[:, mine]),
    )
    load_w = [
        pltpu.make_async_copy(src, dst, loc_sem.at[3 + i]) for i, (src, dst) in enumerate(weight_ends)
    ]
    for copy in load_w:
        copy.start()

    barrier = pltpu.get_barrier_semaphore()
    plane = 2 * n_ep
    here = ep * 2 + c

    def greet(r, carry):
        other = lax.rem(here + r, plane)
        pl.semaphore_signal(
            barrier, inc=1, device_id=device(lax.div(other, 2), 2 * y + lax.rem(other, 2))
        )
        return carry

    with jax.named_scope("greet"):
        lax.fori_loop(1, plane, greet, 0, unroll=9 if plane == 64 else 1)
    pl.semaphore_signal(barrier, inc=1, device_id=device(ep, 2 * right + c))
    pl.semaphore_signal(barrier, inc=1, device_id=device(ep, 2 * left + c))
    flat = ep * n_tp + tp
    total = n_ep * n_tp
    after = lax.rem(flat + 1, total)
    before = lax.rem(flat + total - 1, total)
    after_dev = device(lax.div(after, n_tp), lax.rem(after, n_tp))
    pl.semaphore_signal(barrier, inc=1, device_id=after_dev)
    pl.semaphore_signal(
        barrier, inc=1, device_id=device(lax.div(before, n_tp), lax.rem(before, n_tp))
    )

    with jax.named_scope("routing"):
        small[0].wait()
        small[1].wait()
        chosen = group_ref[...] * EPG + member_ref[...]
        experts = iota((128, tokens), 0)
        named = [chosen[k : k + 1, :] == experts for k in range(2)]
        either = named[0] | named[1]
        upper = jnp.where(
            iota((tokens, tokens), 0) < iota((tokens, tokens), 1), 1.0, 0.0
        ).astype(BF16)
        position = dot(jnp.where(either, 1.0, 0.0).astype(BF16), upper)
        spread = jnp.where(either, position, -1.0).astype(BF16)
        repeat = jnp.where(
            lax.div(iota((slots, 128), 0), HALF) == iota((slots, 128), 1), 1.0, 0.0
        ).astype(BF16)
        wanted = (lax.rem(iota((slots, tokens), 0), HALF) + c * HALF).astype(F32)
        seats = jnp.where(dot(repeat, spread) == wanted, 1.0, 0.0).astype(BF16)

    with jax.named_scope("norm"):
        load_rows.wait()
        small[2].wait()
        square = jnp.zeros((tokens, 128), F32)
        for i in range(width // 128):
            part = rows_v[:, i * 128 : (i + 1) * 128].astype(F32)
            square = square + part * part
        mean = jnp.sum(square, axis=1, keepdims=True) * (1.0 / width)
        scale = lax.rsqrt(mean + 1e-06)

        def seat_rows(k, chunk):
            columns = pl.ds(pl.multiple_of(chunk * CW, CW), CW)
            normed = rows_v[:, columns].astype(F32) * scale * gain_ref[:, columns]
            outb[k] = dot(seats, normed.astype(BF16)).astype(BF16)

        seat_rows(0, y)

    with jax.named_scope("barrier"):
        pl.semaphore_wait(barrier, plane - 1 + 4)

    def offset(j):
        return jnp.where(lax.rem(j, 2) == 1, lax.div(j + 1, 2), lax.rem(n_ep - lax.div(j, 2), n_ep))

    def block(j):
        return pl.ds(pl.multiple_of(j * HALF, HALF), HALF)

    near = steps - 1
    far = lax.rem(y + steps, ny)
    ahead = lax.rem(y + near, ny)
    behind = lax.rem(y + ny - near, ny)

    def hand_over(k, row, chunk, j):
        e = lax.rem(ep + offset(j), n_ep)
        pltpu.make_async_remote_copy(
            src_ref=outb.at[row, block(e)],
            dst_ref=xbuf.at[chunk, block(j)],
            send_sem=d_send.at[k],
            recv_sem=d_recv.at[k, lax.div(j, per_sub)],
            device_id=device(e, tp),
        ).start()

    def dispatch(j, carry):
        hand_over(0, 0, y, j)
        return carry

    def dispatch_more(j, carry):
        odd = lax.rem(lax.div(j, per_sub), 2)
        hand_over(1, 1, far, j)
        hand_over(2, 2 + odd, lax.rem(y + near + odd * (ny - 2 * near) + ny, ny), j)
        return carry

    def keep(k, row, chunk):
        pltpu.make_async_copy(
            outb.at[row, block(ep)], xbuf.at[chunk, block(0)], d_recv.at[k, 0]
        ).start()

    with jax.named_scope("dispatch"):
        lax.fori_loop(1, n_ep, dispatch, 0)
        keep(0, 0, y)
        seat_rows(1, far)
        seat_rows(2, ahead)
        seat_rows(3, behind)
        lax.fori_loop(1, n_ep, dispatch_more, 0)
        keep(1, 1, far)
        keep(2, 2, ahead)

    edge = pltpu.make_async_remote_copy(
        src_ref=kv_hbm.at[:, pl.ds(length - WINDOW, WINDOW), :],
        dst_ref=kv_v.at[:, pl.ds(0, WINDOW), :],
        send_sem=edge_sem.at[0],
        recv_sem=edge_sem.at[1],
        device_id=after_dev,
    )
    edge.start()
    partner = device(ep, 2 * y + 1 - c)
    share_w = [
        pltpu.make_async_remote_copy(
            src_ref=src,
            dst_ref=dst,
            send_sem=w_send.at[i],
            recv_sem=w_recv.at[i],
            device_id=partner,
        )
        for i, (src, dst) in enumerate(weight_ends)
    ]
    with jax.named_scope("shares"):
        for copy in share_w:
            copy.start()

    with jax.named_scope("pick"):
        small[3].wait()
        sheet_v[0:2, :] = weight_ref[...]
        for k in range(2):
            seat = jnp.sum(jnp.where(named[k], position, 0.0), axis=0, keepdims=True)
            sheet_v[2 + k : 3 + k, :] = chosen[k : k + 1, :].astype(F32) * CAP + seat
        sheet_v[4:8, :] = jnp.zeros((4, tokens), F32)
        put_sheet = pltpu.make_async_copy(sheet_v, sheet_out, loc_sem.at[12])
        put_sheet.start()

    gap = lax.rem(iota((2 * WINDOW, 2 * WINDOW), 0), WINDOW) + WINDOW - iota((2 * WINDOW, 2 * WINDOW), 1)
    maskb[...] = jnp.where((gap >= 0) & (gap < WINDOW), 0.0, -1e30)
    with jax.named_scope("loads"):
        load_q.wait()
        load_kv.wait()
        small[4].wait()

    def attend(b, p):
        rows = pl.ds(pl.multiple_of(b * WINDOW, WINDOW), WINDOW)
        key_rows = pl.ds(pl.multiple_of(b * WINDOW, WINDOW), 2 * WINDOW)
        pair = pl.ds(pl.multiple_of(p * 128, 128), 128)
        keys = kv_v[0, key_rows, pair]
        vals = kv_v[1, key_rows, pair]
        low_lane = iota((2 * WINDOW, 128), 1) < HD
        swap = jnp.where(
            lax.rem(iota((128, 128), 0) + HD, 128) == iota((128, 128), 1), 1.0, 0.0
        ).astype(BF16)
        zero = jnp.zeros((2 * WINDOW, 128), BF16)
        keys_sw = dot(keys, swap).astype(BF16)
        vals_sw = dot(vals, swap).astype(BF16)
        start = jnp.where((b == 0) & (flat == 0), -1e30, 0.0)
        visible = maskb[...] + jnp.where(iota((1, 2 * WINDOW), 1) < WINDOW, start, 0.0)
        for h in range(2):
            k_low, k_high = (keys, keys_sw) if h == 0 else (keys_sw, keys)
            v_low, v_high = (vals, vals_sw) if h == 0 else (vals_sw, vals)
            k_half = (jnp.where(low_lane, k_low, zero), jnp.where(low_lane, zero, k_high))
            v_half = (jnp.where(low_lane, v_low, zero), jnp.where(low_lane, zero, v_high))
            at = p * (8 * HD) + h * (4 * HD)
            tiles = [pl.ds(pl.multiple_of(at + i * 128, 128), 128) for i in range(2)]
            query = jnp.concatenate([q_v[rows, t] for t in tiles], axis=0)
            summed = None
            totals = []
            for i in range(2):
                scores = dot_t(query, k_half[i]) * (HD**-0.5) + visible
                head = p * 8 + h * 4 + i
                sink = jnp.where(
                    iota((2 * WINDOW, 1), 0) < WINDOW, sink_ref[head], sink_ref[head + 2]
                )
                highest = jnp.maximum(jnp.max(scores, axis=1, keepdims=True), sink)
                weights = jnp.exp(scores - highest)
                totals.append(jnp.sum(weights, axis=1, keepdims=True) + jnp.exp(sink - highest))
                part = dot(weights.astype(BF16), v_half[i])
                summed = part if summed is None else summed + part
            out = (summed / jnp.where(low_lane, totals[0], totals[1])).astype(BF16)
            for i in range(2):
                att_v[rows, tiles[i]] = out[i * WINDOW : (i + 1) * WINDOW]

    def attend_next(i):
        if i < 2 * blocks:
            b, p = (i // 2 + 1) % blocks, i % 2
            if b == 0 and p == 0:
                edge.wait_recv()
            attend(b, p)
        if i == 2 * blocks - 1:
            pltpu.make_async_copy(att_v, att_out, loc_sem.at[6]).start()

    def piece(buf, phase, way, t, sub, incoming):
        hop = t + 1 if incoming else t
        chunk = lax.rem(y + (ny - hop if way == 0 else hop), ny)
        part = buf.at[chunk, pl.ds(sub * sr, sr)]
        target = right if way == 0 else left
        return pltpu.make_async_remote_copy(
            src_ref=part,
            dst_ref=part,
            send_sem=ring_send.at[phase, way, t, sub],
            recv_sem=ring_recv.at[phase, way, t, sub],
            device_id=device(ep, 2 * target + c),
        )

    lasts = (steps - 2, steps - 1)

    def travels(phase, way, t, sub):
        if t == lasts[phase]:
            return (sub % 2 == 0) == (way == 0)
        return t < lasts[phase]

    def send(buf, phase, t, sub):
        for way in range(2):
            if travels(phase, way, t, sub):
                piece(buf, phase, way, t, sub, False).start()

    def add_chunk(buf, weights, total_ref, chunk, first=False):
        value = dot(buf[chunk], weights[pl.ds(pl.multiple_of(chunk * CW, CW), CW), :])
        if first:
            total_ref[...] = value
        else:
            total_ref[...] += value

    def ring(buf, weights, total_ref, phase, between):
        add_chunk(buf, weights, total_ref, y, True)
        for t in range(lasts[phase]):
            for sub in range(NSUB):
                for way in range(2):
                    piece(buf, phase, way, t, sub, True).wait_recv()
                    if travels(phase, way, t + 1, sub):
                        piece(buf, phase, way, t + 1, sub, False).start()
            between(t)
            add_chunk(buf, weights, total_ref, lax.rem(y + ny - t - 1, ny))
            add_chunk(buf, weights, total_ref, lax.rem(y + t + 1, ny))

    def last_piece(buf, phase, sub):
        way = sub % 2
        piece(buf, phase, way, lasts[phase], sub, True).wait_recv()

    def rows_of(chunk):
        return pl.ds(pl.multiple_of(chunk * CW, CW), CW)

    def landed(k, chunk, sub):
        held = xbuf.at[chunk, pl.ds(sub * sr, sr)]
        pltpu.make_async_copy(held, held, d_recv.at[k, sub]).wait()

    def hide(sub):
        landed(1, far, sub)
        landed(2, ahead if sub % 2 == 0 else behind, sub)
        last_piece(xbuf, 0, sub)
        rows = pl.ds(sub * sr, sr)
        both = acc[rows, :]
        for chunk in (far, ahead, behind):
            both = both + dot(xbuf[chunk, rows], wgu[rows_of(chunk), :])
        gate = both[:, :CW]
        hbuf[y, rows] = (gate / (1.0 + jnp.exp(-gate)) * both[:, CW:]).astype(BF16)
        send(hbuf, 1, 0, sub)

    def give_back(j, carry):
        s = lax.rem(ep + n_ep - offset(j), n_ep)
        theirs = pl.ds(pl.multiple_of((1 - c) * 128, 128), 128)
        pltpu.make_async_remote_copy(
            src_ref=obuf.at[block(j), theirs],
            dst_ref=rbuf.at[back_rows],
            send_sem=r_send.at[0],
            recv_sem=r_recv.at[0],
            device_id=device(s, 2 * y + 1 - c),
        ).start()

        @pl.when(s != ep)
        def _():
            pltpu.make_async_remote_copy(
                src_ref=obuf.at[block(j), mine],
                dst_ref=rbuf.at[back_rows],
                send_sem=r_send.at[1],
                recv_sem=r_recv.at[0],
                device_id=device(s, tp),
            ).start()

        @pl.when(s == ep)
        def _():
            pltpu.make_async_copy(
                obuf.at[block(j), mine], rbuf.at[back_rows], r_recv.at[0]
            ).start()

        return carry

    back_rows = pl.ds(pl.multiple_of(ep * CAP + c * HALF, HALF), HALF)

    def finish(sub):
        last_piece(hbuf, 1, sub)
        rows = pl.ds(sub * sr, sr)
        obuf[rows, :] = (acc2[rows, :] + dot(hbuf[far, rows], wd[rows_of(far), :])).astype(BF16)
        lax.fori_loop(sub * per_sub, (sub + 1) * per_sub, give_back, 0)

    def arrive(sub):
        landed(0, y, sub)
        send(xbuf, 0, 0, sub)

    with jax.named_scope("arrive"):
        arrive(0)
        for sub in range(1, NSUB):
            attend_next(sub - 1)
            arrive(sub)
    with jax.named_scope("weights"):
        for i in range(2):
            load_w[i].wait()
            share_w[i].wait_recv()
    with jax.named_scope("ringx"):
        ring(xbuf, wgu, acc, 0, lambda t: attend_next(NSUB - 1 + t))
    with jax.named_scope("middle"):
        for sub in range(NSUB):
            hide(sub)
    load_w[2].wait()
    share_w[2].wait_recv()
    with jax.named_scope("ringh"):
        ring(hbuf, wd, acc2, 1, lambda t: attend_next(NSUB - 1 + lasts[0] + t))
        for i in range(NSUB - 1 + lasts[0] + lasts[1], 2 * blocks):
            attend_next(i)
    with jax.named_scope("down"):
        for sub in range(NSUB):
            finish(sub)

    with jax.named_scope("close"):
        for phase, buf in ((0, xbuf), (1, hbuf)):
            for way in range(2):
                for t in range(steps):
                    for sub in range(NSUB):
                        if travels(phase, way, t, sub):
                            piece(buf, phase, way, t, sub, False).wait_send()
        sent = outb.at[0, pl.ds(0, slots - HALF)]
        for k in range(3):
            pltpu.make_async_copy(sent, sent, d_send.at[k]).wait()
        edge.wait_send()
        for copy in share_w:
            copy.wait_send()
        pltpu.make_async_copy(att_v, att_out, loc_sem.at[6]).wait()

    with jax.named_scope("home"):
        pltpu.make_async_copy(rbuf, rbuf, r_recv.at[0]).wait()
    put_sheet.wait()
    back = obuf.at[:, pl.ds(0, 128)]
    pltpu.make_async_copy(back, back, r_send.at[0]).wait()
    back_less = obuf.at[pl.ds(0, slots - HALF), pl.ds(0, 128)]
    pltpu.make_async_copy(back_less, back_less, r_send.at[1]).wait()


def hand_on(att_in, back_in, sheet_in, att_out, mix_out, att_v, back_v, sheet_v, mix_v, sem):
    pieces = 4
    size = att_v.shape[0] // pieces
    load_sheet = pltpu.make_async_copy(sheet_in, sheet_v, sem.at[0, 4])
    load_back = pltpu.make_async_copy(back_in, back_v, sem.at[0, 5])
    load_sheet.start()
    load_back.start()
    loads, stores = [], []
    for i in range(pieces):
        part = pl.ds(i * size, size)
        loads.append(pltpu.make_async_copy(att_in.at[part], att_v.at[part], sem.at[0, i]))
        stores.append(pltpu.make_async_copy(att_v.at[part], att_out.at[part], sem.at[1, i]))
    for load in loads:
        load.start()
    load_sheet.wait()
    sheet = sheet_v[...].T
    shape = (sheet.shape[0], back_v.shape[0])
    picks = [
        jnp.where(sheet[:, 2 + k : 3 + k].astype(jnp.int32) == iota(shape, 1), 1.0, 0.0).astype(BF16)
        for k in range(2)
    ]
    load_back.wait()
    mixed = sheet[:, 0:1] * dot(picks[0], back_v[...])
    mix_v[...] = (mixed + sheet[:, 1:2] * dot(picks[1], back_v[...])).astype(BF16)
    put = pltpu.make_async_copy(mix_v, mix_out, sem.at[1, 4])
    put.start()
    for load, store in zip(loads, stores):
        load.wait()
        store.start()
    for store in stores:
        store.wait()
    put.wait()


def shards(
    n_ep,
    n_tp,
    queries,
    keys_values,
    sink_logits,
    moe_rows,
    norm_gain,
    group_choice,
    member_choice,
    route_weight,
    w_gate,
    w_up,
    w_down,
):
    tokens, width = moe_rows.shape
    length = queries.shape[0]
    slots = n_ep * HALF
    ny = n_tp // 2
    steps = ny // 2
    hbm = pl.BlockSpec(memory_space=pl.ANY)
    dma = pltpu.SemaphoreType.DMA
    attended, returned, sheet = pl.pallas_call(
        functools.partial(kernel, n_ep, n_tp),
        out_shape=(
            jax.ShapeDtypeStruct(queries.shape, BF16),
            jax.ShapeDtypeStruct((n_ep * CAP, 128), BF16),
            jax.ShapeDtypeStruct((8, tokens), F32),
        ),
        in_specs=[hbm] * 11,
        out_specs=(hbm, hbm, hbm),
        scratch_shapes=[
            pltpu.SMEM((QH,), F32),
            pltpu.VMEM((1, width), F32),
            pltpu.VMEM((1, tokens), jnp.int32),
            pltpu.VMEM((2, tokens), jnp.int32),
            pltpu.VMEM((2, tokens), F32),
            pltpu.VMEM((tokens, width), BF16),
            pltpu.VMEM((length, QH * HD), BF16),
            pltpu.VMEM((2, length + WINDOW, KVH * HD), BF16),
            pltpu.VMEM((width, 2 * CW), BF16),
            pltpu.VMEM((width, CW), BF16),
            pltpu.VMEM((4, slots, CW), BF16),
            pltpu.VMEM((ny, slots, CW), BF16),
            pltpu.VMEM((ny, slots, CW), BF16),
            pltpu.VMEM((slots, 2 * CW), F32),
            pltpu.VMEM((slots, CW), F32),
            pltpu.VMEM((slots, CW), BF16),
            pltpu.VMEM((length, QH * HD), BF16),
            pltpu.VMEM((2 * WINDOW, 2 * WINDOW), F32),
            pltpu.VMEM((8, tokens), F32),
            dma((13,)),
            dma((3,)),
            dma((3,)),
            dma((2,)),
            dma((3,)),
            dma((3, NSUB)),
            dma((2, 2, steps, NSUB)),
            dma((2, 2, steps, NSUB)),
            dma((2,)),
            dma((1,)),
        ],
        compiler_params=pltpu.CompilerParams(
            collective_id=0, has_side_effects=True, vmem_limit_bytes=66900000
        ),
        name="step",
    )(
        queries,
        keys_values,
        sink_logits,
        moe_rows,
        norm_gain.reshape(1, width),
        group_choice.reshape(1, tokens),
        member_choice.T,
        route_weight.T,
        w_gate,
        w_up,
        w_down,
    )
    return pl.pallas_call(
        hand_on,
        out_shape=(
            jax.ShapeDtypeStruct(attended.shape, BF16),
            jax.ShapeDtypeStruct((tokens, 128), BF16),
        ),
        in_specs=[hbm, hbm, hbm],
        out_specs=(hbm, hbm),
        scratch_shapes=[
            pltpu.VMEM(attended.shape, BF16),
            pltpu.VMEM(returned.shape, BF16),
            pltpu.VMEM(sheet.shape, F32),
            pltpu.VMEM((tokens, 128), BF16),
            dma((2, 6)),
        ],
        compiler_params=pltpu.CompilerParams(vmem_limit_bytes=66900000),
        name="hand_on",
    )(attended, returned, sheet)


def solution(mesh):
    in_specs = (
        P(("ep", "tp"), None),
        P(None, ("ep", "tp"), None),
        P(),
        P("ep", None),
        P(),
        P("ep"),
        P("ep", None),
        P("ep", None),
        P("ep", None, "tp"),
        P("ep", None, "tp"),
        P("ep", None, "tp"),
    )
    out_specs = (P(("ep", "tp"), None), P("ep", "tp"))
    body = functools.partial(shards, mesh.shape["ep"], mesh.shape["tp"])
    return jax.shard_map(body, mesh=mesh, in_specs=in_specs, out_specs=out_specs, check_vma=False)
```
